32 devices in a mesh: ep: 8 (over z, x), tp: 4 (over y, core).
Axes of the slice: x: 2, y: 2, z: 4, core: 2. Of those that a mesh axis runs over, the one named last changes fastest.
Arguments:
- queries: bfloat16 [2048, 1024], P('ep', 'tp'), may hold values from -6 to 6
- keys: bfloat16 [2048, 256], P('ep', 'tp'), may hold values from -6 to 6
- values: bfloat16 [2048, 256], P('ep', 'tp'), may hold values from -6 to 6
- q_gain: float32 [64], replicated, may hold values from 1 to 6
- k_gain: float32 [64], replicated, may hold values from 1 to 6
- out_weight: bfloat16 [1024, 2048], P('tp'), may hold values from -0.1875 to 0.1875
- tokens: bfloat16 [1024, 2048], P(('ep', 'tp')), may hold values from -6 to 6
- ffn_gain: float32 [2048], replicated, may hold values from 0.1 to 1.9
- route: int32 [1024, 2], P(('ep', 'tp')), may hold values from 0 to 7, all different within a row; in each aligned block of 32 rows (0 to 31, 32 to 63, ...) at most 16 rows name the same one
- route_weight: float32 [1024, 2], P(('ep', 'tp')), may hold values from 0.1 to 1
- gate_weight: bfloat16 [8, 2048, 3584], P('ep', None, 'tp'), may hold values from -0.125 to 0.125
- up_weight: bfloat16 [8, 2048, 3584], P('ep', None, 'tp'), may hold values from -0.125 to 0.125
- down_weight: bfloat16 [8, 3584, 2048], P('ep', 'tp'), may hold values from -0.09375 to 0.09375
Outputs:
- mixer_out: bfloat16 [2048, 2048], P(('ep', 'tp'))
- mixed: bfloat16 [1024, 2048], P(('ep', 'tp'))
The draws below stay inside these ranges and needn't reach their ends.
Inputs may be any that keep to these rules, and one draw needn't show every extreme that they name: `route`: each row names 2 different experts. In every device's aligned block of 32 rows no expert is named more than 16 times, and in some blocks some expert is named exactly 16 times.
All inputs are finite; a program needn't handle non-finite values.
Results may differ from the reference program's by a relative error of at most 0.013.
The reference program's roundings to bfloat16 on the way count: a program that leaves them out, or rounds other values in their place, can miss the bound.
Values may be sent and summed in bfloat16 or wider, within the bound.
No kernel may reach another device: no remote copies, remote signals or barrier semaphores. Data moves between devices by JAX's collectives and lax.ppermute only.
A program may use at most 192 MiB of HBM per device.

```python
import math
import jax
import jax.numpy as jnp
import numpy as np
from jax import lax

D = 2048
HEADS = 16
KV_HEADS = 4
HEAD_DIM = 64
FF = 3584
TOPK = 2
GRID_W = 64
TOKENS_A = 2048
TOKENS_B = 1024
EXPERTS = 8
ROUTE_ROWS = 32
CAPACITY = 16
QW = 1024
KVW = 256
N_TP = 4


def draw_gain(key, salt):
    inner = jax.random.fold_in(key, salt)
    logs = jax.random.uniform(inner, (HEAD_DIM,), jnp.float32, 0.0, math.log(2.5))
    return jnp.exp(logs)


def draw_q_gain(key, part):
    return draw_gain(key, 21)


def draw_k_gain(key, part):
    return draw_gain(key, 22)


def draw_pair(key):
    query_key = jax.random.fold_in(key, 41)
    key_key = jax.random.fold_in(key, 42)
    query_vals = jnp.clip(jax.random.normal(query_key, (TOKENS_A, HEADS, HEAD_DIM), jnp.float32), -6.0, 6.0)
    key_vals = jnp.clip(jax.random.normal(key_key, (TOKENS_A, KV_HEADS, HEAD_DIM), jnp.float32), -6.0, 6.0)
    return (query_vals.reshape(TOKENS_A, HEADS * HEAD_DIM), key_vals.reshape(TOKENS_A, KV_HEADS * HEAD_DIM))


def draw_queries(key, part):
    return draw_pair(key)[0].astype(jnp.bfloat16)


def draw_keys(key, part):
    return draw_pair(key)[1].astype(jnp.bfloat16)


def block_levels(own_key, extent, shards, smallest, top_value):
    loudness = 1.0
    for position, blocks in shards:
        heights = jax.random.uniform(jax.random.fold_in(jax.random.fold_in(own_key, 6), position), (blocks,), jnp.float32, smallest / len(shards), top_value / len(shards))
        loudness = loudness * jnp.repeat(jnp.exp(heights), extent[position] // blocks).reshape((-1,) + (1,) * (len(extent) - 1 - position))
    return loudness


def assign_block(stream_key, own, number, rows, amount, top, reach, skew):
    order = jax.random.permutation(stream_key, amount)
    crowded, usual = portions_of(amount, rows * top, reach, skew, True), portions_of(amount, rows * top, reach, skew, False)
    places = jnp.arange(amount)

    def named(sizes, turn):
        used = int((sizes > 0).sum())
        fixed = max(1, used // 4)
        passed = fixed + (places - fixed + turn * (used - fixed)) % max(1, amount - fixed)
        return jnp.zeros((amount,), jnp.int32).at[order[jnp.where(places < fixed, places, passed)]].set(jnp.asarray(sizes, jnp.int32))

    sizes = jnp.where(number % 4 == 0, named(crowded, number // 4), named(usual, number - number // 4 - 1))
    mixed = jax.random.permutation(jax.random.fold_in(own, 3), amount)
    source_of, sink = mixed[0:amount // 2 * 2:2], mixed[1:amount // 2 * 2:2]
    slack = jnp.minimum(sizes[source_of] - 1, reach - sizes[sink]) // 2
    slack = jnp.where((source_of == order[0]) | (sink == order[0]) | (sizes[sink] == 0), 0, jnp.maximum(slack, 0))
    passed = jax.random.randint(jax.random.fold_in(own, 4), (amount // 2,), 0, 1 << 20) % (slack + 1)
    sizes = sizes.at[source_of].add(-passed).at[sink].add(passed)
    items = jnp.searchsorted(jnp.cumsum(sizes), jnp.arange(rows * top), side="right").astype(jnp.int32)
    grid = items.reshape(top, rows).T
    grid = grid[jax.random.permutation(jax.random.fold_in(own, 1), rows)]
    turn = jax.random.randint(jax.random.fold_in(own, 2), (rows, 1), 0, top)
    return jnp.take_along_axis(grid, (jnp.arange(top)[None, :] + turn) % top, axis=1)


def portions_of(number_of, total, reach, slope, full):
    portions = [(1 << 20) // math.isqrt(rank ** slope) + 1 for rank in range(1, number_of + 1)]
    largest = reach if full else min(reach, max(-(-total // number_of), total * portions[0] // sum(portions)))
    least = 1 if total - largest >= number_of - 1 else 0
    counts, surplus = [largest] + [least] * (number_of - 1), total - largest - least * (number_of - 1)
    while surplus > 0:
        movable = [i for i in range(1, number_of) if counts[i] < largest] or [i for i in range(1, number_of) if counts[i] < reach]
        mass, remaining = sum([portions[i] for i in movable]), surplus
        for i in movable:
            addition = min(reach - counts[i], max(1, remaining * portions[i] // mass), surplus)
            counts[i] = counts[i] + addition
            surplus = surplus - addition
    return np.array(counts)


def normal_values(own_key, extent, scale, most, cuts=(), kind=jnp.bfloat16):
    entries = scale * jax.random.normal(own_key, extent, jnp.float32)
    if cuts:
        entries = entries * block_levels(own_key, extent, cuts, -0.22, 0.18)
    return jnp.clip(entries, -most, most).astype(kind)


def setup_inputs(seed: int = 0) -> dict:
    splits = jax.random.split(jax.random.key(seed), 14)
    queries = draw_queries(jax.random.fold_in(splits[13], 71), 0)
    keys = draw_keys(jax.random.fold_in(splits[13], 71), 0)
    values = normal_values(splits[2], (TOKENS_A, KVW), 1.0, 6.0, ((0, 8), (1, 4)))
    q_gain = draw_q_gain(jax.random.fold_in(splits[13], 71), 0)
    k_gain = draw_k_gain(jax.random.fold_in(splits[13], 71), 0)
    out_weight = normal_values(splits[5], (QW, D), QW ** -0.5, 0.1875, ((0, 4),))
    tokens = normal_values(splits[6], (TOKENS_B, D), 1.0, 6.0, ((0, 32),))
    ffn_gain = jnp.clip(1.0 + 0.18 * jax.random.normal(splits[7], (D,), jnp.float32), 0.1, 1.9)
    route_keys = jax.random.split(jax.random.fold_in(splits[8], 1), TOKENS_B // ROUTE_ROWS)
    route_turns = jax.random.permutation(jax.random.fold_in(splits[8], 3), TOKENS_B // ROUTE_ROWS)
    route = jax.vmap(lambda own, number: assign_block(jax.random.fold_in(splits[8], 2), own, number, ROUTE_ROWS, EXPERTS, TOPK, CAPACITY, 1))(route_keys, route_turns).reshape((TOKENS_B, TOPK))
    route_weight = jnp.clip(0.1 + 0.9 * jax.random.uniform(splits[9], (TOKENS_B, TOPK), jnp.float32) ** block_levels(splits[9], (TOKENS_B, TOPK), ((0, 32),), -0.2, 0.2), 0.1, 1.0)
    gate_weight = normal_values(splits[10], (EXPERTS, D, FF), D ** -0.5, 0.125, ((0, 8), (2, 4)))
    up_weight = normal_values(splits[11], (EXPERTS, D, FF), D ** -0.5, 0.125, ((0, 8), (2, 4)))
    down_weight = normal_values(splits[12], (EXPERTS, FF, D), FF ** -0.5, 0.09375, ((0, 8), (1, 4)))
    return dict(queries=queries, keys=keys, values=values, q_gain=q_gain, k_gain=k_gain, out_weight=out_weight, tokens=tokens, ffn_gain=ffn_gain, route=route, route_weight=route_weight, gate_weight=gate_weight, up_weight=up_weight, down_weight=down_weight)


EPS = 1e-06
THETA = 10000.0

def head_norm(vals, gain):
    vals = vals.astype(jnp.float32)
    return vals * lax.rsqrt(lax.optimization_barrier(jnp.mean(vals * vals, axis=-1, keepdims=True)) + EPS) * gain

def rotate(vals, positions):
    pairs = vals.shape[-1] // 2
    quarter = pairs // 2
    freqs = THETA ** (-jnp.arange(quarter, dtype=jnp.float32) / quarter)
    grid_row = (positions // GRID_W).astype(jnp.float32)
    grid_col = (positions % GRID_W).astype(jnp.float32)
    angle = jnp.concatenate([grid_row[:, None] * freqs, grid_col[:, None] * freqs], axis=-1)
    cosine = jnp.cos(angle)[:, None, :]
    sine = jnp.sin(angle)[:, None, :]
    split = vals.reshape(vals.shape[:-1] + (pairs, 2))
    first = split[..., 0]
    second = split[..., 1]
    turned = jnp.stack([first * cosine - second * sine, first * sine + second * cosine], axis=-1)
    return turned.reshape(vals.shape)

def reference(queries, keys, values, q_gain, k_gain, out_weight, tokens, ffn_gain, route, route_weight, gate_weight, up_weight, down_weight):
    total = queries.shape[0]
    group = HEADS // KV_HEADS
    positions = jnp.arange(total, dtype=jnp.int32)
    rot_q = rotate(head_norm(queries.reshape(total, HEADS, HEAD_DIM), q_gain), positions).astype(jnp.bfloat16)
    rot_k = rotate(head_norm(keys.reshape(total, KV_HEADS, HEAD_DIM), k_gain), positions).astype(jnp.bfloat16)
    key_float = rot_k.astype(jnp.float32)
    value_float = values.reshape(total, KV_HEADS, HEAD_DIM).astype(jnp.float32)
    scale = HEAD_DIM ** (-0.5)
    block = math.gcd(total, 256)

    def attend(query_block):
        scores = jnp.einsum('qkgd,skd->qkgs', query_block.astype(jnp.float32), key_float) * scale
        highest = lax.optimization_barrier(jnp.max(scores, axis=-1, keepdims=True))
        expo = jnp.exp(scores - highest)
        denom = lax.optimization_barrier(jnp.sum(expo, axis=-1))
        probs = lax.optimization_barrier(expo.astype(jnp.bfloat16)).astype(jnp.float32)
        numer = jnp.einsum('qkgs,skd->qkgd', probs, value_float)
        return (numer / denom[..., None]).astype(jnp.bfloat16)
    query_blocks = rot_q.reshape(total // block, block, KV_HEADS, group, HEAD_DIM)
    attended = lax.map(attend, query_blocks).reshape(total, QW)
    share = QW // N_TP
    summed = jnp.zeros((total, D), jnp.float32)
    for index in range(N_TP):
        part = jnp.dot(attended[:, index * share:(index + 1) * share], out_weight[index * share:(index + 1) * share], preferred_element_type=jnp.float32)
        summed = summed + part.astype(jnp.bfloat16).astype(jnp.float32)
    mixer_out = summed.astype(jnp.bfloat16)
    token_float = tokens.astype(jnp.float32)
    normed = (token_float * lax.rsqrt(lax.optimization_barrier(jnp.mean(token_float * token_float, axis=-1, keepdims=True)) + EPS) * ffn_gain).astype(jnp.bfloat16)
    picks = route.reshape(-1)
    count = picks.shape[0]
    limit = tokens.shape[0] // ROUTE_ROWS * CAPACITY
    hidden_share = FF // N_TP

    def one_expert(expert):
        order = jnp.argsort((picks != expert).astype(jnp.int32), stable=True)[:limit].astype(jnp.int32)
        valid = picks[order] == expert
        chosen = normed[order // TOPK]
        gate = jnp.dot(chosen, gate_weight[expert], preferred_element_type=jnp.float32)
        upper = jnp.dot(chosen, up_weight[expert], preferred_element_type=jnp.float32)
        hidden = (jax.nn.silu(gate) * upper).astype(jnp.bfloat16)
        down = down_weight[expert]
        result = jnp.zeros((limit, D), jnp.float32)
        for index in range(N_TP):
            part = jnp.dot(hidden[:, index * hidden_share:(index + 1) * hidden_share], down[index * hidden_share:(index + 1) * hidden_share], preferred_element_type=jnp.float32)
            result = result + part.astype(jnp.bfloat16).astype(jnp.float32)
        target = jnp.where(valid, order, count).astype(jnp.int32)
        return (result.astype(jnp.bfloat16), target)
    outputs, targets = lax.map(one_expert, jnp.arange(EXPERTS, dtype=jnp.int32))
    per_pick = jnp.zeros((count, D), jnp.bfloat16).at[targets.reshape(-1)].set(outputs.reshape(-1, D), mode='drop')
    weighted = route_weight[..., None] * per_pick.reshape(tokens.shape[0], TOPK, D).astype(jnp.float32)
    mixed = lax.optimization_barrier(jnp.sum(weighted, axis=1)).astype(jnp.bfloat16)
    return (mixer_out, mixed)
```

```python
import functools

import jax
import jax.numpy as jnp
import numpy as np
from jax import lax
from jax.experimental import pallas as pl
from jax.experimental.pallas import tpu as pltpu
from jax.sharding import Mesh
from jax.sharding import PartitionSpec as P

GRID_W = 64
EPS = 1e-06
THETA = 10000.0
LANES = 128
DIRECT_MAX = 8
FLOPS_PER_MICRO = 5e8

WHOLE = "whole"
VMEM = pl.BlockSpec(memory_space=pltpu.VMEM)
SMEM = pl.BlockSpec(memory_space=pltpu.SMEM)
ANY = pl.BlockSpec(memory_space=pltpu.HBM)
MIB = 1024 * 1024


def in_hbm(vals):
    return pltpu.with_memory_space_constraint(vals, pltpu.HBM)


def call(body, outs, in_specs, args, scratch=(), micros=1.0, mib=6):
    def whole(shape):
        return pl.BlockSpec(shape, lambda i: (0,) * len(shape))

    return pl.pallas_call(
        body,
        grid=(1,),
        out_shape=[jax.ShapeDtypeStruct(s, d) for s, d in outs],
        in_specs=[whole(a.shape) if t is WHOLE else t for t, a in zip(in_specs, args)],
        out_specs=[VMEM for _ in outs],
        scratch_shapes=list(scratch),
        compiler_params=pltpu.CompilerParams(vmem_limit_bytes=mib * MIB),
        cost_estimate=pl.CostEstimate(
            flops=int(micros * FLOPS_PER_MICRO), bytes_accessed=0, transcendentals=0
        ),
    )(*[in_hbm(a) if t is WHOLE or t is ANY else a for t, a in zip(in_specs, args)])


def swap(vals, axis, distance=1):
    size = lax.axis_size(axis)
    return lax.ppermute(vals, axis, [(i, i ^ distance) for i in range(size)])


def exchange(vals, capacity):
    shape = vals.shape
    vals = vals.reshape(-1, capacity, shape[1])
    vals = lax.all_to_all(vals, ("n", "y"), split_axis=0, concat_axis=0, tiled=True)
    return vals.reshape(shape)


def pick_hots(meta, base, near, sides, capacity, top):
    rows = meta.shape[0]
    lane = lax.broadcasted_iota(jnp.int32, (rows, LANES), 1).astype(jnp.float32)
    chosen = [meta[:, k : k + 1] for k in range(top)]
    hots = [(c == lane).astype(jnp.float32) for c in chosen]
    count = functools.reduce(jnp.add, hots)
    lower = (
        lax.broadcasted_iota(jnp.int32, (rows, rows), 0)
        > lax.broadcasted_iota(jnp.int32, (rows, rows), 1)
    ).astype(jnp.float32)
    prior = jnp.dot(lower, count, preferred_element_type=jnp.float32)
    total = near * sides * capacity
    spot = lax.broadcasted_iota(jnp.int32, (rows, total), 1)
    spot = (spot // (sides * capacity) * capacity + spot % capacity).astype(jnp.float32)
    out = []
    for k in range(top):
        rank = jnp.sum(hots[k] * prior, axis=1, keepdims=True)
        for j in range(k):
            rank = rank + (chosen[j] == chosen[k]).astype(jnp.float32)
        own = chosen[k] - base
        inside = (own >= 0.0) & (own < float(near))
        slot = jnp.where(inside, own * float(capacity) + rank, -1.0)
        out.append((slot == spot).astype(jnp.float32))
    return out


def spread(hots, normed):
    row_hot = functools.reduce(jnp.add, hots).astype(jnp.bfloat16)
    out = lax.dot_general(
        row_hot, normed, (((0,), (0,)), ((), ())), preferred_element_type=jnp.float32
    )
    return out.astype(jnp.bfloat16)


def send_body(base_ref, tok_ref, gain_ref, route_ref, weight_ref, far_ref, near_ref, *, sizes):
    top = sizes[-1]
    width = tok_ref.shape[1]
    own = tok_ref.shape[0]
    eye = lax.broadcasted_iota(jnp.int32, (own, own), 0) == lax.broadcasted_iota(
        jnp.int32, (own, own), 1
    )

    def column(row):
        return jnp.sum(jnp.where(eye, row, 0.0), axis=1, keepdims=True)

    vals = tok_ref[...].astype(jnp.float32)
    normed = vals * lax.rsqrt(jnp.mean(vals * vals, axis=-1, keepdims=True) + EPS) * gain_ref[...]
    normed = normed.astype(jnp.bfloat16)
    far_ref[:, :width] = normed
    lane = lax.broadcasted_iota(jnp.int32, (vals.shape[0], LANES), 1)
    meta = jnp.zeros((vals.shape[0], LANES), jnp.float32)
    for k in range(top):
        weight = column(weight_ref[k : k + 1, :])
        high = weight.astype(jnp.bfloat16).astype(jnp.float32)
        rest = weight - high
        middle = rest.astype(jnp.bfloat16).astype(jnp.float32)
        pieces = (column(route_ref[k : k + 1, :].astype(jnp.float32)), high, middle, rest - middle)
        for i, piece in enumerate(pieces):
            meta = jnp.where(lane == i * top + k, piece, meta)
    far_ref[:, width:] = meta.astype(jnp.bfloat16)
    hots = pick_hots(meta, base_ref[0].astype(jnp.float32), *sizes)
    near_ref[...] = spread(hots, normed)


def relay_body(base_ref, far_ref, out_ref, *, sizes):
    width = out_ref.shape[1]
    meta = far_ref[:, width:].astype(jnp.float32)
    hots = pick_hots(meta, base_ref[0].astype(jnp.float32), *sizes)
    out_ref[...] = spread(hots, far_ref[:, :width])


def collect_body(base_ref, meta_ref, back_ref, out_ref, *, sizes):
    top = sizes[-1]
    meta = meta_ref[:, out_ref.shape[1] :].astype(jnp.float32)
    hots = pick_hots(meta, base_ref[0].astype(jnp.float32), *sizes)
    back = back_ref[...]
    total = None
    for k in range(top):
        rows = jnp.dot(hots[k].astype(jnp.bfloat16), back, preferred_element_type=jnp.float32)
        rows = rows.astype(jnp.bfloat16).astype(jnp.float32)
        weight = meta[:, top + k : top + k + 1] + (
            meta[:, 2 * top + k : 2 * top + k + 1] + meta[:, 3 * top + k : 3 * top + k + 1]
        )
        total = weight * rows if total is None else total + weight * rows
    out_ref[...] = total.astype(out_ref.dtype)


def expert_body(
    mine_ref, other_ref, gate_hbm, up_hbm, down_hbm, mine_out, other_out, gate, up, down, sems
):
    copies = [
        pltpu.make_async_copy(src.at[0], dst, sems.at[i])
        for i, (src, dst) in enumerate(((gate_hbm, gate), (up_hbm, up), (down_hbm, down)))
    ]
    for copy in copies:
        copy.start()
    rows = jnp.concatenate([mine_ref[...], other_ref[...]], axis=0)
    count = mine_ref.shape[0]
    copies[0].wait()
    lhs = jnp.dot(rows, gate[...], preferred_element_type=jnp.float32)
    copies[1].wait()
    rhs = jnp.dot(rows, up[...], preferred_element_type=jnp.float32)
    hidden = (lhs / (1.0 + jnp.exp(-lhs)) * rhs).astype(jnp.bfloat16)
    copies[2].wait()
    out = jnp.dot(hidden, down[...], preferred_element_type=jnp.float32).astype(jnp.bfloat16)
    mine_out[...] = out[:count]
    other_out[...] = out[count:]


def add_body(left_ref, right_ref, out_ref):
    total = left_ref[...].astype(jnp.float32) + right_ref[...].astype(jnp.float32)
    out_ref[...] = total.astype(out_ref.dtype)


def run_expert(mine, other, gate_weight, up_weight, down_weight):
    count, width = mine.shape
    inner = gate_weight.shape[2]
    bf16 = jnp.bfloat16
    return call(
        expert_body,
        [((count, width), bf16), ((count, width), bf16)],
        [VMEM, VMEM, ANY, ANY, ANY],
        (mine, other, gate_weight, up_weight, down_weight),
        [
            pltpu.VMEM((width, inner), bf16),
            pltpu.VMEM((width, inner), bf16),
            pltpu.VMEM((inner, width), bf16),
            pltpu.SemaphoreType.DMA((3,)),
        ],
        micros=5.0,
        mib=24,
    )


def turn_tables(rows_total, head_size):
    quarter = head_size // 4
    freqs = THETA ** (-np.arange(quarter, dtype=np.float64) / quarter)
    sign = np.where(np.arange(head_size // 2) % 2 == 0, -1.0, 1.0)

    def table(count, first):
        angle = np.repeat(np.arange(count, dtype=np.float64)[:, None] * freqs, 2, axis=1)
        zero = np.zeros_like(angle)
        out = []
        for part in (np.cos(angle), np.sin(angle) * sign):
            halves = [part, zero] if first else [zero, part]
            out.append(np.concatenate(halves, axis=1))
        return np.stack(out).astype(np.float32)

    return table(rows_total, True), table(GRID_W, False)


def qkv_body(start_ref, q_ref, k_ref, v_ref, qg_ref, kg_ref, row_ref, col_ref, _, q_out, kv_out):
    rows, q_width = q_ref.shape
    k_width = k_ref.shape[0]
    head = qg_ref.shape[1]
    span = q_width + k_width
    unit = (
        lax.broadcasted_iota(jnp.int32, (k_width, k_width), 0)
        == lax.broadcasted_iota(jnp.int32, (k_width, k_width), 1)
    ).astype(jnp.bfloat16)

    def upright(ref):
        return lax.dot_general(
            ref[...], unit, (((0,), (0,)), ((), ())), preferred_element_type=jnp.float32
        )

    vals = jnp.concatenate([q_ref[...].astype(jnp.float32), upright(k_ref)], axis=1)
    gain = jnp.concatenate([qg_ref[...]] * (q_width // head) + [kg_ref[...]] * (k_width // head), 1)
    same = (
        lax.broadcasted_iota(jnp.int32, (span, span), 0) // head
        == lax.broadcasted_iota(jnp.int32, (span, span), 1) // head
    ).astype(jnp.float32)
    power = jnp.dot(
        vals * vals, same, preferred_element_type=jnp.float32, precision=lax.Precision.HIGHEST
    )
    vals = vals * lax.rsqrt(power * (1.0 / head) + EPS) * gain
    even = lax.broadcasted_iota(jnp.int32, (rows, span), 1) % 2 == 0
    left = jnp.concatenate([vals[:, 1:], vals[:, :1]], axis=1)
    right = jnp.concatenate([vals[:, span - 1 :], vals[:, : span - 1]], axis=1)
    partner = jnp.where(even, left, right)
    turned = []
    for i in range(rows // GRID_W):
        at = start_ref[0] + i
        cosine = row_ref[0, pl.ds(at, 1), :] + col_ref[0]
        sine = row_ref[1, pl.ds(at, 1), :] + col_ref[1]
        cosine = jnp.concatenate([cosine] * (span // head), axis=1)
        sine = jnp.concatenate([sine] * (span // head), axis=1)
        low = i * GRID_W
        high = low + GRID_W
        turned.append(vals[low:high] * cosine + partner[low:high] * sine)
    turned = jnp.concatenate(turned, axis=0).astype(jnp.bfloat16)
    q_out[...] = turned[:, :q_width] * (head**-0.5)
    kv_out[...] = jnp.concatenate(
        [turned[:, q_width:], upright(v_ref).astype(jnp.bfloat16)], axis=1
    )


def attend_body(core_ref, q_ref, *refs, head, key_heads, sides):
    kvs = refs[:-4]
    weight_ref, sent_ref, kept_ref, att = refs[-4:]
    heads = q_ref.shape[1] // head
    for h in range(heads):
        g = h * key_heads // heads
        query = q_ref[:, h * head : (h + 1) * head]
        scores = []
        for kv in kvs:
            scores.append(
                lax.dot_general(
                    query,
                    kv[:, g * head : (g + 1) * head],
                    (((1,), (1,)), ((), ())),
                    preferred_element_type=jnp.float32,
                )
            )
        high = functools.reduce(jnp.maximum, [jnp.max(s, -1, keepdims=True) for s in scores])
        denom = None
        numer = None
        for s, kv in zip(scores, kvs):
            expo = jnp.exp(s - high)
            part = jnp.sum(expo, axis=-1, keepdims=True)
            at = (key_heads + g) * head
            prod = jnp.dot(
                expo.astype(jnp.bfloat16), kv[:, at : at + head], preferred_element_type=jnp.float32
            )
            denom = part if denom is None else denom + part
            numer = prod if numer is None else numer + prod
        att[:, h * head : (h + 1) * head] = (numer / denom).astype(jnp.bfloat16)
    share = q_ref.shape[0] // (2 * sides)
    core = core_ref[0]
    for out_ref, which in ((sent_ref, 1 - core), (kept_ref, core)):
        rows = jnp.concatenate(
            [att[pl.ds(pl.multiple_of((2 * s + which) * share, share), share), :] for s in range(sides)]
        )
        out = jnp.dot(rows, weight_ref[...], preferred_element_type=jnp.float32)
        out_ref[...] = out.astype(jnp.bfloat16)


def attend_blocks(rot_q, joined, key_heads, head):
    rows = rot_q.shape[0]
    group = rot_q.shape[1] // head // key_heads
    queries = rot_q.reshape(rows, key_heads, group, head)
    width = key_heads * head

    def fold_block(carry, block):
        highest, denom, numer = carry
        key_block = block[:, :width].reshape(-1, key_heads, head)
        value_block = block[:, width:].reshape(-1, key_heads, head)
        scores = jnp.einsum("qkgd,skd->qkgs", queries, key_block, preferred_element_type=jnp.float32)
        new_high = jnp.maximum(highest, jnp.max(scores, axis=-1))
        shrink = jnp.exp(highest - new_high)
        expo = jnp.exp(scores - new_high[..., None])
        denom = denom * shrink + jnp.sum(expo, axis=-1)
        numer = numer * shrink[..., None] + jnp.einsum(
            "qkgs,skd->qkgd",
            expo.astype(jnp.bfloat16),
            value_block,
            preferred_element_type=jnp.float32,
        )
        return ((new_high, denom, numer), None)

    shape = (rows, key_heads, group)
    carry = (
        jnp.full(shape, -1e30, jnp.float32),
        jnp.zeros(shape, jnp.float32),
        jnp.zeros(shape + (head,), jnp.float32),
    )
    length = joined.shape[0]
    size = length
    while size > 2048 and size % 2 == 0:
        size = size // 2
    blocks = joined.reshape(length // size, size, joined.shape[1])
    carry, _ = lax.scan(fold_block, carry, blocks)
    _, denom, numer = carry
    return (numer / denom[..., None]).astype(jnp.bfloat16).reshape(rows, -1)


def attention(rot_q, joined, out_weight, key_heads, head):
    near = lax.axis_size("n")
    sides = lax.axis_size("y")
    core = lax.axis_index("c").astype(jnp.int32)
    rows = rot_q.shape[0]
    width = out_weight.shape[1]
    far = swap(joined, "f")
    if near <= DIRECT_MAX:
        pair = jnp.concatenate([joined, far], axis=0)
        kvs = [pair] + [swap(pair, "n", k) for k in range(1, near)]
        body = functools.partial(attend_body, head=head, key_heads=key_heads, sides=sides)
        half = ((rows // 2, width), jnp.bfloat16)
        return call(
            body,
            [half, half],
            [SMEM] + [VMEM] * (len(kvs) + 1) + [WHOLE],
            (core.reshape(1), rot_q, *kvs, out_weight),
            [pltpu.VMEM(rot_q.shape, jnp.bfloat16)],
            micros=5.0,
            mib=24,
        )
    pair = jnp.concatenate([joined, far], axis=0)
    joined = lax.all_gather(pair, "n", axis=0, tiled=True)
    attended = attend_blocks(rot_q, joined, key_heads, head)
    blocks = attended.reshape(sides, 2, -1, attended.shape[1])

    def project(which):
        part = lax.dynamic_index_in_dim(blocks, which, 1, False).reshape(rows // 2, -1)
        out = jnp.dot(part, out_weight, preferred_element_type=jnp.float32)
        return out.astype(jnp.bfloat16)

    return project(1 - core), project(core)


def finish_mixer(sent, kept):
    sides = lax.axis_size("y")
    pair = kept.astype(jnp.float32) + swap(sent, "c").astype(jnp.float32)
    pair = pair.reshape(sides, -1, kept.shape[1])
    if sides == 1:
        return pair[0].astype(jnp.bfloat16)
    if sides == 2:
        side = lax.axis_index("y")
        sent = lax.dynamic_index_in_dim(pair, 1 - side, 0, False).astype(jnp.bfloat16)
        kept = lax.dynamic_index_in_dim(pair, side, 0, False)
        return (kept + swap(sent, "y").astype(jnp.float32)).astype(jnp.bfloat16)
    moved = lax.all_to_all(pair.astype(jnp.bfloat16), "y", 0, 0, tiled=True)
    return jnp.sum(moved.astype(jnp.float32), axis=0).astype(jnp.bfloat16)


def local(
    queries,
    keys,
    values,
    q_gain,
    k_gain,
    out_weight,
    tokens,
    ffn_gain,
    route,
    route_weight,
    gate_weight,
    up_weight,
    down_weight,
):
    bf16 = jnp.bfloat16
    near = lax.axis_size("n")
    sides = lax.axis_size("y")
    half = lax.axis_index("f").astype(jnp.int32)
    here = half * near + lax.axis_index("n").astype(jnp.int32)
    base = (half * near).reshape(1)

    own_rows, width = tokens.shape
    top = route.shape[1]
    capacity = own_rows * top // near
    sizes = (near, sides, capacity, top)
    slots = near * sides * capacity
    send = functools.partial(send_body, sizes=sizes)
    outgoing, near_rows = call(
        send, [((own_rows, width + LANES), bf16), ((slots, width), bf16)], [SMEM] + [WHOLE] * 4,
        (base, tokens, ffn_gain.reshape(1, -1), route.T, route_weight.T), micros=1.5)
    far = swap(outgoing, "f")
    near_in = exchange(near_rows, capacity)
    relay = functools.partial(relay_body, sizes=sizes)
    (far_rows,) = call(relay, [((slots, width), bf16)], [SMEM, VMEM], (base, far))
    far_in = exchange(far_rows, capacity)

    local_rows = queries.shape[0]
    head = q_gain.shape[0]
    row_table, col_table = turn_tables(local_rows * 2 * near // GRID_W, head)
    rot_q, joined = call(
        qkv_body,
        [(queries.shape, bf16), ((local_rows, 2 * keys.shape[1]), bf16)],
        [SMEM] + [WHOLE] * 7 + [VMEM],
        (
            (here * (local_rows // GRID_W)).reshape(1),
            queries,
            keys.T,
            values.T,
            q_gain.reshape(1, -1),
            k_gain.reshape(1, -1),
            row_table,
            col_table,
            near_rows,
        ),
        micros=1.5,
    )

    weights = (gate_weight, up_weight, down_weight)

    def work(rows):
        mine, other = run_expert(rows, swap(rows, "c"), *weights)
        args = (mine, swap(other, "c"))
        return call(add_body, [(rows.shape, bf16)], [VMEM] * 2, args)[0]

    near_out = work(near_in)
    far_out = work(far_in)
    far_back = exchange(far_out, capacity)
    near_back = exchange(near_out, capacity)

    sent, kept = attention(rot_q, joined, out_weight, keys.shape[1] // head, head)
    mixer_out = finish_mixer(sent, kept)

    collect = functools.partial(collect_body, sizes=sizes)

    def gather_back(meta, back, dtype):
        return call(
            collect, [((own_rows, width), dtype)], [SMEM, VMEM, VMEM], (base, meta, back)
        )[0]

    far_sum = swap(gather_back(far, far_back, bf16), "f")
    near_sum = gather_back(outgoing, near_back, jnp.float32)
    mixed = (near_sum + far_sum.astype(jnp.float32)).astype(bf16)
    return (mixer_out, mixed)


def solution(mesh):
    devices = mesh.devices
    groups, parts = devices.shape
    split = Mesh(devices.reshape(2, groups // 2, parts // 2, 2), ("f", "n", "y", "c"))
    ep = ("f", "n")
    tp = ("y", "c")
    placed = (
        P(ep, tp),
        P(ep, tp),
        P(ep, tp),
        P(),
        P(),
        P(tp, None),
        P(ep + tp, None),
        P(),
        P(ep + tp, None),
        P(ep + tp, None),
        P(ep, None, tp),
        P(ep, None, tp),
        P(ep, tp, None),
    )
    return jax.shard_map(
        local,
        mesh=split,
        in_specs=placed,
        out_specs=(P(ep + tp, None), P(ep + tp, None)),
        check_vma=False,
    )
```

```python
import functools

import jax
import jax.numpy as jnp
import numpy as np
from jax import lax
from jax.experimental import pallas as pl
from jax.experimental.pallas import tpu as pltpu
from jax.sharding import Mesh
from jax.sharding import PartitionSpec as P

GRID_W = 64
EPS = 1e-06
THETA = 10000.0
LANES = 128
DIRECT_MAX = 8
FLOPS_PER_MICRO = 5e8
GATE_CUT = 512

WHOLE = "whole"
VMEM = pl.BlockSpec(memory_space=pltpu.VMEM)
SMEM = pl.BlockSpec(memory_space=pltpu.SMEM)
ANY = pl.BlockSpec(memory_space=pltpu.HBM)
MIB = 1024 * 1024


def in_hbm(vals):
    return pltpu.with_memory_space_constraint(vals, pltpu.HBM)


def call(body, outs, in_specs, args, scratch=(), micros=1.0, mib=6):
    def whole(shape):
        return pl.BlockSpec(shape, lambda i: (0,) * len(shape))

    return pl.pallas_call(
        body,
        grid=(1,),
        out_shape=[jax.ShapeDtypeStruct(s, d) for s, d in outs],
        in_specs=[whole(a.shape) if t is WHOLE else t for t, a in zip(in_specs, args)],
        out_specs=[VMEM for _ in outs],
        scratch_shapes=list(scratch),
        compiler_params=pltpu.CompilerParams(vmem_limit_bytes=mib * MIB),
        cost_estimate=pl.CostEstimate(
            flops=int(micros * FLOPS_PER_MICRO), bytes_accessed=0, transcendentals=0
        ),
    )(*[in_hbm(a) if t is WHOLE or t is ANY else a for t, a in zip(in_specs, args)])


def swap(vals, axis, distance=1):
    size = lax.axis_size(axis)
    return lax.ppermute(vals, axis, [(i, i ^ distance) for i in range(size)])


def exchange(vals, capacity):
    shape = vals.shape
    vals = vals.reshape(-1, capacity, shape[1])
    vals = lax.all_to_all(vals, ("n", "y"), split_axis=0, concat_axis=0, tiled=True)
    return vals.reshape(shape)


def pick_hots(meta, base, near, sides, capacity, top):
    rows = meta.shape[0]
    lane = lax.broadcasted_iota(jnp.int32, (rows, LANES), 1).astype(jnp.float32)
    chosen = [meta[:, k : k + 1] for k in range(top)]
    hots = [(c == lane).astype(jnp.float32) for c in chosen]
    count = functools.reduce(jnp.add, hots)
    lower = (
        lax.broadcasted_iota(jnp.int32, (rows, rows), 0)
        > lax.broadcasted_iota(jnp.int32, (rows, rows), 1)
    ).astype(jnp.float32)
    prior = jnp.dot(lower, count, preferred_element_type=jnp.float32)
    total = near * sides * capacity
    spot = lax.broadcasted_iota(jnp.int32, (rows, total), 1)
    spot = (spot // (sides * capacity) * capacity + spot % capacity).astype(jnp.float32)
    out = []
    for k in range(top):
        rank = jnp.sum(hots[k] * prior, axis=1, keepdims=True)
        for j in range(k):
            rank = rank + (chosen[j] == chosen[k]).astype(jnp.float32)
        own = chosen[k] - base
        inside = (own >= 0.0) & (own < float(near))
        slot = jnp.where(inside, own * float(capacity) + rank, -1.0)
        out.append((slot == spot).astype(jnp.float32))
    return out


def spread(hots, normed):
    row_hot = functools.reduce(jnp.add, hots).astype(jnp.bfloat16)
    out = lax.dot_general(
        row_hot, normed, (((0,), (0,)), ((), ())), preferred_element_type=jnp.float32
    )
    return out.astype(jnp.bfloat16)


def send_body(base_ref, tok_ref, gain_ref, route_ref, weight_ref, far_ref, near_ref, *, sizes):
    top = sizes[-1]
    width = tok_ref.shape[1]
    own = tok_ref.shape[0]
    eye = lax.broadcasted_iota(jnp.int32, (own, own), 0) == lax.broadcasted_iota(
        jnp.int32, (own, own), 1
    )

    def column(row):
        return jnp.sum(jnp.where(eye, row, 0.0), axis=1, keepdims=True)

    vals = tok_ref[...].astype(jnp.float32)
    normed = vals * lax.rsqrt(jnp.mean(vals * vals, axis=-1, keepdims=True) + EPS) * gain_ref[...]
    normed = normed.astype(jnp.bfloat16)
    far_ref[:, :width] = normed
    lane = lax.broadcasted_iota(jnp.int32, (vals.shape[0], LANES), 1)
    meta = jnp.zeros((vals.shape[0], LANES), jnp.float32)
    for k in range(top):
        weight = column(weight_ref[k : k + 1, :])
        high = weight.astype(jnp.bfloat16).astype(jnp.float32)
        rest = weight - high
        middle = rest.astype(jnp.bfloat16).astype(jnp.float32)
        pieces = (column(route_ref[k : k + 1, :].astype(jnp.float32)), high, middle, rest - middle)
        for i, piece in enumerate(pieces):
            meta = jnp.where(lane == i * top + k, piece, meta)
    far_ref[:, width:] = meta.astype(jnp.bfloat16)
    hots = pick_hots(meta, base_ref[0].astype(jnp.float32), *sizes)
    near_ref[...] = spread(hots, normed)


def relay_body(base_ref, far_ref, out_ref, *, sizes):
    width = out_ref.shape[1]
    meta = far_ref[:, width:].astype(jnp.float32)
    hots = pick_hots(meta, base_ref[0].astype(jnp.float32), *sizes)
    out_ref[...] = spread(hots, far_ref[:, :width])


def collect_body(base_ref, meta_ref, back_ref, out_ref, *, sizes):
    top = sizes[-1]
    meta = meta_ref[:, out_ref.shape[1] :].astype(jnp.float32)
    hots = pick_hots(meta, base_ref[0].astype(jnp.float32), *sizes)
    back = back_ref[...]
    total = None
    for k in range(top):
        rows = jnp.dot(hots[k].astype(jnp.bfloat16), back, preferred_element_type=jnp.float32)
        rows = rows.astype(jnp.bfloat16).astype(jnp.float32)
        weight = meta[:, top + k : top + k + 1] + (
            meta[:, 2 * top + k : 2 * top + k + 1] + meta[:, 3 * top + k : 3 * top + k + 1]
        )
        total = weight * rows if total is None else total + weight * rows
    out_ref[...] = total.astype(out_ref.dtype)


def cuts(total, step):
    return [(i, min(step, total - i)) for i in range(0, total, step)]


def expert_body(
    mine_ref, other_ref, gate_hbm, up_hbm, down_hbm, mine_out, other_out, gate, up, down, sems
):
    spans = cuts(gate.shape[1], GATE_CUT)
    copies = [
        pltpu.make_async_copy(
            gate_hbm.at[0, :, pl.ds(at, size)], gate.at[:, pl.ds(at, size)], sems.at[i]
        )
        for i, (at, size) in enumerate(spans)
    ]
    copies.append(pltpu.make_async_copy(up_hbm.at[0], up, sems.at[len(spans)]))
    copies.append(pltpu.make_async_copy(down_hbm.at[0], down, sems.at[len(spans) + 1]))
    for copy in copies:
        copy.start()
    rows = jnp.concatenate([mine_ref[...], other_ref[...]], axis=0)
    count = mine_ref.shape[0]
    parts = []
    for copy, (at, size) in zip(copies, spans):
        copy.wait()
        parts.append(jnp.dot(rows, gate[:, at : at + size], preferred_element_type=jnp.float32))
    lhs = jnp.concatenate(parts, axis=1)
    copies[-2].wait()
    rhs = jnp.dot(rows, up[...], preferred_element_type=jnp.float32)
    hidden = (lhs / (1.0 + jnp.exp(-lhs)) * rhs).astype(jnp.bfloat16)
    copies[-1].wait()
    out = jnp.dot(hidden, down[...], preferred_element_type=jnp.float32).astype(jnp.bfloat16)
    mine_out[...] = out[:count]
    other_out[...] = out[count:]


def add_body(left_ref, right_ref, out_ref):
    total = left_ref[...].astype(jnp.float32) + right_ref[...].astype(jnp.float32)
    out_ref[...] = total.astype(out_ref.dtype)


def run_expert(mine, other, gate_weight, up_weight, down_weight):
    count, width = mine.shape
    inner = gate_weight.shape[2]
    bf16 = jnp.bfloat16
    return call(
        expert_body,
        [((count, width), bf16), ((count, width), bf16)],
        [VMEM, VMEM, ANY, ANY, ANY],
        (mine, other, gate_weight, up_weight, down_weight),
        [
            pltpu.VMEM((width, inner), bf16),
            pltpu.VMEM((width, inner), bf16),
            pltpu.VMEM((inner, width), bf16),
            pltpu.SemaphoreType.DMA((len(cuts(inner, GATE_CUT)) + 2,)),
        ],
        micros=5.0,
        mib=24,
    )


def turn_tables(rows_total, head_size):
    quarter = head_size // 4
    freqs = THETA ** (-np.arange(quarter, dtype=np.float64) / quarter)
    sign = np.where(np.arange(head_size // 2) % 2 == 0, -1.0, 1.0)

    def table(count, first):
        angle = np.repeat(np.arange(count, dtype=np.float64)[:, None] * freqs, 2, axis=1)
        zero = np.zeros_like(angle)
        out = []
        for part in (np.cos(angle), np.sin(angle) * sign):
            halves = [part, zero] if first else [zero, part]
            out.append(np.concatenate(halves, axis=1))
        return np.stack(out).astype(np.float32)

    return table(rows_total, True), table(GRID_W, False)


def qkv_body(start_ref, q_ref, k_ref, v_ref, qg_ref, kg_ref, row_ref, col_ref, _, q_out, kv_out):
    rows, q_width = q_ref.shape
    k_width = k_ref.shape[0]
    head = qg_ref.shape[1]
    span = q_width + k_width
    unit = (
        lax.broadcasted_iota(jnp.int32, (k_width, k_width), 0)
        == lax.broadcasted_iota(jnp.int32, (k_width, k_width), 1)
    ).astype(jnp.bfloat16)

    def upright(ref):
        return lax.dot_general(
            ref[...], unit, (((0,), (0,)), ((), ())), preferred_element_type=jnp.float32
        )

    vals = jnp.concatenate([q_ref[...].astype(jnp.float32), upright(k_ref)], axis=1)
    gain = jnp.concatenate([qg_ref[...]] * (q_width // head) + [kg_ref[...]] * (k_width // head), 1)
    same = (
        lax.broadcasted_iota(jnp.int32, (span, span), 0) // head
        == lax.broadcasted_iota(jnp.int32, (span, span), 1) // head
    ).astype(jnp.float32)
    power = jnp.dot(
        vals * vals, same, preferred_element_type=jnp.float32, precision=lax.Precision.HIGHEST
    )
    vals = vals * lax.rsqrt(power * (1.0 / head) + EPS) * gain
    even = lax.broadcasted_iota(jnp.int32, (rows, span), 1) % 2 == 0
    left = jnp.concatenate([vals[:, 1:], vals[:, :1]], axis=1)
    right = jnp.concatenate([vals[:, span - 1 :], vals[:, : span - 1]], axis=1)
    partner = jnp.where(even, left, right)
    turned = []
    for i in range(rows // GRID_W):
        at = start_ref[0] + i
        cosine = row_ref[0, pl.ds(at, 1), :] + col_ref[0]
        sine = row_ref[1, pl.ds(at, 1), :] + col_ref[1]
        cosine = jnp.concatenate([cosine] * (span // head), axis=1)
        sine = jnp.concatenate([sine] * (span // head), axis=1)
        low = i * GRID_W
        high = low + GRID_W
        turned.append(vals[low:high] * cosine + partner[low:high] * sine)
    turned = jnp.concatenate(turned, axis=0).astype(jnp.bfloat16)
    q_out[...] = turned[:, :q_width] * (head**-0.5)
    kv_out[...] = jnp.concatenate(
        [turned[:, q_width:], upright(v_ref).astype(jnp.bfloat16)], axis=1
    )


def attend_body(core_ref, q_ref, *refs, head, key_heads, sides):
    kvs = refs[:-4]
    weight_ref, sent_ref, kept_ref, att = refs[-4:]
    heads = q_ref.shape[1] // head
    for h in range(heads):
        g = h * key_heads // heads
        query = q_ref[:, h * head : (h + 1) * head]
        scores = []
        for kv in kvs:
            scores.append(
                lax.dot_general(
                    query,
                    kv[:, g * head : (g + 1) * head],
                    (((1,), (1,)), ((), ())),
                    preferred_element_type=jnp.float32,
                )
            )
        high = functools.reduce(jnp.maximum, [jnp.max(s, -1, keepdims=True) for s in scores])
        denom = None
        numer = None
        for s, kv in zip(scores, kvs):
            expo = jnp.exp(s - high)
            part = jnp.sum(expo, axis=-1, keepdims=True)
            at = (key_heads + g) * head
            prod = jnp.dot(
                expo.astype(jnp.bfloat16), kv[:, at : at + head], preferred_element_type=jnp.float32
            )
            denom = part if denom is None else denom + part
            numer = prod if numer is None else numer + prod
        att[:, h * head : (h + 1) * head] = (numer / denom).astype(jnp.bfloat16)
    share = q_ref.shape[0] // (2 * sides)
    core = core_ref[0]
    for out_ref, which in ((sent_ref, 1 - core), (kept_ref, core)):
        rows = jnp.concatenate(
            [att[pl.ds(pl.multiple_of((2 * s + which) * share, share), share), :] for s in range(sides)]
        )
        out = jnp.dot(rows, weight_ref[...], preferred_element_type=jnp.float32)
        out_ref[...] = out.astype(jnp.bfloat16)


def attend_blocks(rot_q, joined, key_heads, head):
    rows = rot_q.shape[0]
    group = rot_q.shape[1] // head // key_heads
    queries = rot_q.reshape(rows, key_heads, group, head)
    width = key_heads * head

    def fold_block(carry, block):
        highest, denom, numer = carry
        key_block = block[:, :width].reshape(-1, key_heads, head)
        value_block = block[:, width:].reshape(-1, key_heads, head)
        scores = jnp.einsum("qkgd,skd->qkgs", queries, key_block, preferred_element_type=jnp.float32)
        new_high = jnp.maximum(highest, jnp.max(scores, axis=-1))
        shrink = jnp.exp(highest - new_high)
        expo = jnp.exp(scores - new_high[..., None])
        denom = denom * shrink + jnp.sum(expo, axis=-1)
        numer = numer * shrink[..., None] + jnp.einsum(
            "qkgs,skd->qkgd",
            expo.astype(jnp.bfloat16),
            value_block,
            preferred_element_type=jnp.float32,
        )
        return ((new_high, denom, numer), None)

    shape = (rows, key_heads, group)
    carry = (
        jnp.full(shape, -1e30, jnp.float32),
        jnp.zeros(shape, jnp.float32),
        jnp.zeros(shape + (head,), jnp.float32),
    )
    length = joined.shape[0]
    size = length
    while size > 2048 and size % 2 == 0:
        size = size // 2
    blocks = joined.reshape(length // size, size, joined.shape[1])
    carry, _ = lax.scan(fold_block, carry, blocks)
    _, denom, numer = carry
    return (numer / denom[..., None]).astype(jnp.bfloat16).reshape(rows, -1)


def attention(rot_q, joined, out_weight, key_heads, head):
    near = lax.axis_size("n")
    sides = lax.axis_size("y")
    core = lax.axis_index("c").astype(jnp.int32)
    rows = rot_q.shape[0]
    width = out_weight.shape[1]
    far = swap(joined, "f")
    if near <= DIRECT_MAX:
        pair = jnp.concatenate([joined, far], axis=0)
        kvs = [pair]
        for k in [1 << b for b in reversed(range(near.bit_length() - 1))]:
            held = kvs[0] if len(kvs) == 1 else jnp.concatenate(kvs, axis=0)
            kvs = [held, swap(held, "n", k)]
        body = functools.partial(attend_body, head=head, key_heads=key_heads, sides=sides)
        half = ((rows // 2, width), jnp.bfloat16)
        return call(
            body,
            [half, half],
            [SMEM, WHOLE] + [VMEM] * len(kvs) + [WHOLE],
            (core.reshape(1), rot_q, *kvs, out_weight),
            [pltpu.VMEM(rot_q.shape, jnp.bfloat16)],
            micros=5.0,
            mib=24,
        )
    pair = jnp.concatenate([joined, far], axis=0)
    joined = lax.all_gather(pair, "n", axis=0, tiled=True)
    attended = attend_blocks(rot_q, joined, key_heads, head)
    blocks = attended.reshape(sides, 2, -1, attended.shape[1])

    def project(which):
        part = lax.dynamic_index_in_dim(blocks, which, 1, False).reshape(rows // 2, -1)
        out = jnp.dot(part, out_weight, preferred_element_type=jnp.float32)
        return out.astype(jnp.bfloat16)

    return project(1 - core), project(core)


def finish_mixer(sent, kept):
    sides = lax.axis_size("y")
    pair = kept.astype(jnp.float32) + swap(sent, "c").astype(jnp.float32)
    pair = pair.reshape(sides, -1, kept.shape[1])
    if sides == 1:
        return pair[0].astype(jnp.bfloat16)
    if sides == 2:
        side = lax.axis_index("y")
        sent = lax.dynamic_index_in_dim(pair, 1 - side, 0, False).astype(jnp.bfloat16)
        kept = lax.dynamic_index_in_dim(pair, side, 0, False)
        return (kept + swap(sent, "y").astype(jnp.float32)).astype(jnp.bfloat16)
    moved = lax.all_to_all(pair.astype(jnp.bfloat16), "y", 0, 0, tiled=True)
    return jnp.sum(moved.astype(jnp.float32), axis=0).astype(jnp.bfloat16)


def local(
    queries,
    keys,
    values,
    q_gain,
    k_gain,
    out_weight,
    tokens,
    ffn_gain,
    route,
    route_weight,
    gate_weight,
    up_weight,
    down_weight,
):
    bf16 = jnp.bfloat16
    near = lax.axis_size("n")
    sides = lax.axis_size("y")
    half = lax.axis_index("f").astype(jnp.int32)
    here = half * near + lax.axis_index("n").astype(jnp.int32)
    base = (half * near).reshape(1)

    own_rows, width = tokens.shape
    top = route.shape[1]
    capacity = own_rows * top // near
    sizes = (near, sides, capacity, top)
    slots = near * sides * capacity
    send = functools.partial(send_body, sizes=sizes)
    outgoing, near_rows = call(
        send, [((own_rows, width + LANES), bf16), ((slots, width), bf16)], [SMEM] + [WHOLE] * 4,
        (base, tokens, ffn_gain.reshape(1, -1), route.T, route_weight.T), micros=1.5)
    far = swap(outgoing, "f")
    near_in = exchange(near_rows, capacity)
    relay = functools.partial(relay_body, sizes=sizes)
    (far_rows,) = call(relay, [((slots, width), bf16)], [SMEM, VMEM], (base, far))
    far_in = exchange(far_rows, capacity)

    local_rows = queries.shape[0]
    head = q_gain.shape[0]
    row_table, col_table = turn_tables(local_rows * 2 * near // GRID_W, head)
    rot_q, joined = call(
        qkv_body,
        [(queries.shape, bf16), ((local_rows, 2 * keys.shape[1]), bf16)],
        [SMEM] + [WHOLE] * 7 + [VMEM],
        (
            (here * (local_rows // GRID_W)).reshape(1),
            queries,
            keys.T,
            values.T,
            q_gain.reshape(1, -1),
            k_gain.reshape(1, -1),
            row_table,
            col_table,
            near_rows,
        ),
        micros=1.5,
    )

    weights = (gate_weight, up_weight, down_weight)

    def work(rows):
        mine, other = run_expert(rows, swap(rows, "c"), *weights)
        args = (mine, swap(other, "c"))
        return call(add_body, [(rows.shape, bf16)], [VMEM] * 2, args)[0]

    near_out = work(near_in)
    far_out = work(far_in)
    far_back = exchange(far_out, capacity)
    near_back = exchange(near_out, capacity)

    sent, kept = attention(rot_q, joined, out_weight, keys.shape[1] // head, head)
    mixer_out = finish_mixer(sent, kept)

    collect = functools.partial(collect_body, sizes=sizes)

    def gather_back(meta, back, dtype):
        return call(
            collect, [((own_rows, width), dtype)], [SMEM, VMEM, VMEM], (base, meta, back)
        )[0]

    far_sum = swap(gather_back(far, far_back, bf16), "f")
    near_sum = gather_back(outgoing, near_back, jnp.float32)
    mixed = (near_sum + far_sum.astype(jnp.float32)).astype(bf16)
    return (mixer_out, mixed)


def solution(mesh):
    devices = mesh.devices
    groups, parts = devices.shape
    split = Mesh(devices.reshape(2, groups // 2, parts // 2, 2), ("f", "n", "y", "c"))
    ep = ("f", "n")
    tp = ("y", "c")
    placed = (
        P(ep, tp),
        P(ep, tp),
        P(ep, tp),
        P(),
        P(),
        P(tp, None),
        P(ep + tp, None),
        P(),
        P(ep + tp, None),
        P(ep + tp, None),
        P(ep, None, tp),
        P(ep, None, tp),
        P(ep, tp, None),
    )
    return jax.shard_map(
        local,
        mesh=split,
        in_specs=placed,
        out_specs=(P(ep + tp, None), P(ep + tp, None)),
        check_vma=False,
    )
```

```python
import functools

import jax
import jax.numpy as jnp
import numpy as np
from jax import lax
from jax.experimental import pallas as pl
from jax.experimental.pallas import tpu as pltpu
from jax.sharding import Mesh
from jax.sharding import PartitionSpec as P

GRID_W = 64
EPS = 1e-06
THETA = 10000.0
LANES = 128
DIRECT_MAX = 8
FLOPS_PER_MICRO = 5e8
GATE_CUT = 512

WHOLE = "whole"
VMEM = pl.BlockSpec(memory_space=pltpu.VMEM)
SMEM = pl.BlockSpec(memory_space=pltpu.SMEM)
ANY = pl.BlockSpec(memory_space=pltpu.HBM)
MIB = 1024 * 1024


def in_hbm(vals):
    return pltpu.with_memory_space_constraint(vals, pltpu.HBM)


def call(body, outs, in_specs, args, scratch=(), micros=1.0, mib=6):
    def whole(shape):
        return pl.BlockSpec(shape, lambda i: (0,) * len(shape))

    return pl.pallas_call(
        body,
        grid=(1,),
        out_shape=[jax.ShapeDtypeStruct(s, d) for s, d in outs],
        in_specs=[whole(a.shape) if t is WHOLE else t for t, a in zip(in_specs, args)],
        out_specs=[VMEM for _ in outs],
        scratch_shapes=list(scratch),
        compiler_params=pltpu.CompilerParams(vmem_limit_bytes=mib * MIB),
        cost_estimate=pl.CostEstimate(
            flops=int(micros * FLOPS_PER_MICRO), bytes_accessed=0, transcendentals=0
        ),
    )(*[in_hbm(a) if t is WHOLE or t is ANY else a for t, a in zip(in_specs, args)])


def swap(vals, axis, distance=1):
    size = lax.axis_size(axis)
    return lax.ppermute(vals, axis, [(i, i ^ distance) for i in range(size)])


def exchange(vals, capacity):
    shape = vals.shape
    vals = vals.reshape(-1, capacity, shape[1])
    vals = lax.all_to_all(vals, ("n", "y"), split_axis=0, concat_axis=0, tiled=True)
    return vals.reshape(shape)


def pick_hots(meta, base, near, sides, capacity, top):
    rows = meta.shape[0]
    lane = lax.broadcasted_iota(jnp.int32, (rows, LANES), 1).astype(jnp.float32)
    chosen = [meta[:, k : k + 1] for k in range(top)]
    hots = [(c == lane).astype(jnp.float32) for c in chosen]
    count = functools.reduce(jnp.add, hots)
    lower = (
        lax.broadcasted_iota(jnp.int32, (rows, rows), 0)
        > lax.broadcasted_iota(jnp.int32, (rows, rows), 1)
    ).astype(jnp.float32)
    prior = jnp.dot(lower, count, preferred_element_type=jnp.float32)
    total = near * sides * capacity
    spot = lax.broadcasted_iota(jnp.int32, (rows, total), 1)
    spot = (spot // (sides * capacity) * capacity + spot % capacity).astype(jnp.float32)
    out = []
    for k in range(top):
        rank = jnp.sum(hots[k] * prior, axis=1, keepdims=True)
        for j in range(k):
            rank = rank + (chosen[j] == chosen[k]).astype(jnp.float32)
        own = chosen[k] - base
        inside = (own >= 0.0) & (own < float(near))
        slot = jnp.where(inside, own * float(capacity) + rank, -1.0)
        out.append((slot == spot).astype(jnp.float32))
    return out


def spread(hots, normed):
    row_hot = functools.reduce(jnp.add, hots).astype(jnp.bfloat16)
    out = lax.dot_general(
        row_hot, normed, (((0,), (0,)), ((), ())), preferred_element_type=jnp.float32
    )
    return out.astype(jnp.bfloat16)


def send_body(base_ref, tok_ref, gain_ref, route_ref, weight_ref, far_ref, near_ref, *, sizes):
    top = sizes[-1]
    width = tok_ref.shape[1]
    own = tok_ref.shape[0]
    eye = lax.broadcasted_iota(jnp.int32, (own, own), 0) == lax.broadcasted_iota(
        jnp.int32, (own, own), 1
    )

    def column(row):
        return jnp.sum(jnp.where(eye, row, 0.0), axis=1, keepdims=True)

    vals = tok_ref[...].astype(jnp.float32)
    normed = vals * lax.rsqrt(jnp.mean(vals * vals, axis=-1, keepdims=True) + EPS) * gain_ref[...]
    normed = normed.astype(jnp.bfloat16)
    far_ref[:, :width] = normed
    lane = lax.broadcasted_iota(jnp.int32, (vals.shape[0], LANES), 1)
    meta = jnp.zeros((vals.shape[0], LANES), jnp.float32)
    for k in range(top):
        weight = column(weight_ref[k : k + 1, :])
        high = weight.astype(jnp.bfloat16).astype(jnp.float32)
        rest = weight - high
        middle = rest.astype(jnp.bfloat16).astype(jnp.float32)
        pieces = (column(route_ref[k : k + 1, :].astype(jnp.float32)), high, middle, rest - middle)
        for i, piece in enumerate(pieces):
            meta = jnp.where(lane == i * top + k, piece, meta)
    far_ref[:, width:] = meta.astype(jnp.bfloat16)
    hots = pick_hots(meta, base_ref[0].astype(jnp.float32), *sizes)
    near_ref[...] = spread(hots, normed)


def relay_body(base_ref, far_ref, out_ref, *, sizes):
    width = out_ref.shape[1]
    meta = far_ref[:, width:].astype(jnp.float32)
    hots = pick_hots(meta, base_ref[0].astype(jnp.float32), *sizes)
    out_ref[...] = spread(hots, far_ref[:, :width])


def collect_body(base_ref, meta_ref, back_ref, out_ref, *, sizes):
    top = sizes[-1]
    meta = meta_ref[:, out_ref.shape[1] :].astype(jnp.float32)
    hots = pick_hots(meta, base_ref[0].astype(jnp.float32), *sizes)
    back = back_ref[...]
    total = None
    for k in range(top):
        rows = jnp.dot(hots[k].astype(jnp.bfloat16), back, preferred_element_type=jnp.float32)
        rows = rows.astype(jnp.bfloat16).astype(jnp.float32)
        weight = meta[:, top + k : top + k + 1] + (
            meta[:, 2 * top + k : 2 * top + k + 1] + meta[:, 3 * top + k : 3 * top + k + 1]
        )
        total = weight * rows if total is None else total + weight * rows
    out_ref[...] = total.astype(out_ref.dtype)


def cuts(total, step):
    return [(i, min(step, total - i)) for i in range(0, total, step)]


def expert_body(
    mine_ref, other_ref, gate_hbm, up_hbm, down_hbm, mine_out, other_out, gate, up, down, sems
):
    spans = cuts(gate.shape[1], GATE_CUT)
    copies = [
        pltpu.make_async_copy(
            gate_hbm.at[0, :, pl.ds(at, size)], gate.at[:, pl.ds(at, size)], sems.at[i]
        )
        for i, (at, size) in enumerate(spans)
    ]
    copies.append(pltpu.make_async_copy(up_hbm.at[0], up, sems.at[len(spans)]))
    copies.append(pltpu.make_async_copy(down_hbm.at[0], down, sems.at[len(spans) + 1]))
    for copy in copies:
        copy.start()
    rows = jnp.concatenate([mine_ref[...], other_ref[...]], axis=0)
    count = mine_ref.shape[0]
    parts = []
    for copy, (at, size) in zip(copies, spans):
        copy.wait()
        parts.append(jnp.dot(rows, gate[:, at : at + size], preferred_element_type=jnp.float32))
    copies[-2].wait()
    acts = []
    for lhs, (at, size) in zip(parts, spans):
        rhs = jnp.dot(rows, up[:, at : at + size], preferred_element_type=jnp.float32)
        acts.append((lhs / (1.0 + jnp.exp(-lhs)) * rhs).astype(jnp.bfloat16))
    hidden = jnp.concatenate(acts, axis=1)
    copies[-1].wait()
    out = jnp.dot(hidden, down[...], preferred_element_type=jnp.float32).astype(jnp.bfloat16)
    mine_out[...] = out[:count]
    other_out[...] = out[count:]


def add_body(left_ref, right_ref, out_ref):
    total = left_ref[...].astype(jnp.float32) + right_ref[...].astype(jnp.float32)
    out_ref[...] = total.astype(out_ref.dtype)


def run_expert(mine, other, gate_weight, up_weight, down_weight):
    count, width = mine.shape
    inner = gate_weight.shape[2]
    bf16 = jnp.bfloat16
    return call(
        expert_body,
        [((count, width), bf16), ((count, width), bf16)],
        [VMEM, VMEM, ANY, ANY, ANY],
        (mine, other, gate_weight, up_weight, down_weight),
        [
            pltpu.VMEM((width, inner), bf16),
            pltpu.VMEM((width, inner), bf16),
            pltpu.VMEM((inner, width), bf16),
            pltpu.SemaphoreType.DMA((len(cuts(inner, GATE_CUT)) + 2,)),
        ],
        micros=5.0,
        mib=24,
    )


def turn_tables(rows_total, head_size):
    quarter = head_size // 4
    freqs = THETA ** (-np.arange(quarter, dtype=np.float64) / quarter)
    sign = np.where(np.arange(head_size // 2) % 2 == 0, -1.0, 1.0)

    def table(count, first):
        angle = np.repeat(np.arange(count, dtype=np.float64)[:, None] * freqs, 2, axis=1)
        zero = np.zeros_like(angle)
        out = []
        for part in (np.cos(angle), np.sin(angle) * sign):
            halves = [part, zero] if first else [zero, part]
            out.append(np.concatenate(halves, axis=1))
        return np.stack(out).astype(np.float32)

    return table(rows_total, True), table(GRID_W, False)


def qkv_body(start_ref, q_ref, k_ref, v_ref, qg_ref, kg_ref, row_ref, col_ref, _, q_out, kv_out):
    rows, q_width = q_ref.shape
    k_width = k_ref.shape[0]
    head = qg_ref.shape[1]
    span = q_width + k_width
    unit = (
        lax.broadcasted_iota(jnp.int32, (k_width, k_width), 0)
        == lax.broadcasted_iota(jnp.int32, (k_width, k_width), 1)
    ).astype(jnp.bfloat16)

    def upright(ref):
        return lax.dot_general(
            ref[...], unit, (((0,), (0,)), ((), ())), preferred_element_type=jnp.float32
        )

    vals = jnp.concatenate([q_ref[...].astype(jnp.float32), upright(k_ref)], axis=1)
    gain = jnp.concatenate([qg_ref[...]] * (q_width // head) + [kg_ref[...]] * (k_width // head), 1)
    same = (
        lax.broadcasted_iota(jnp.int32, (span, span), 0) // head
        == lax.broadcasted_iota(jnp.int32, (span, span), 1) // head
    ).astype(jnp.float32)
    power = jnp.dot(
        vals * vals, same, preferred_element_type=jnp.float32, precision=lax.Precision.HIGHEST
    )
    vals = vals * lax.rsqrt(power * (1.0 / head) + EPS) * gain
    even = lax.broadcasted_iota(jnp.int32, (rows, span), 1) % 2 == 0
    left = jnp.concatenate([vals[:, 1:], vals[:, :1]], axis=1)
    right = jnp.concatenate([vals[:, span - 1 :], vals[:, : span - 1]], axis=1)
    partner = jnp.where(even, left, right)
    turned = []
    for i in range(rows // GRID_W):
        at = start_ref[0] + i
        cosine = row_ref[0, pl.ds(at, 1), :] + col_ref[0]
        sine = row_ref[1, pl.ds(at, 1), :] + col_ref[1]
        cosine = jnp.concatenate([cosine] * (span // head), axis=1)
        sine = jnp.concatenate([sine] * (span // head), axis=1)
        low = i * GRID_W
        high = low + GRID_W
        turned.append(vals[low:high] * cosine + partner[low:high] * sine)
    turned = jnp.concatenate(turned, axis=0).astype(jnp.bfloat16)
    q_out[...] = turned[:, :q_width] * (head**-0.5)
    kv_out[...] = jnp.concatenate(
        [turned[:, q_width:], upright(v_ref).astype(jnp.bfloat16)], axis=1
    )


def attend_body(core_ref, q_ref, *refs, head, key_heads, sides):
    kvs = refs[:-4]
    weight_ref, sent_ref, kept_ref, att = refs[-4:]
    heads = q_ref.shape[1] // head
    for h in range(heads):
        g = h * key_heads // heads
        query = q_ref[:, h * head : (h + 1) * head]
        scores = []
        for kv in kvs:
            scores.append(
                lax.dot_general(
                    query,
                    kv[:, g * head : (g + 1) * head],
                    (((1,), (1,)), ((), ())),
                    preferred_element_type=jnp.float32,
                )
            )
        high = functools.reduce(jnp.maximum, [jnp.max(s, -1, keepdims=True) for s in scores])
        denom = None
        numer = None
        for s, kv in zip(scores, kvs):
            expo = jnp.exp(s - high)
            part = jnp.sum(expo, axis=-1, keepdims=True)
            at = (key_heads + g) * head
            prod = jnp.dot(
                expo.astype(jnp.bfloat16), kv[:, at : at + head], preferred_element_type=jnp.float32
            )
            denom = part if denom is None else denom + part
            numer = prod if numer is None else numer + prod
        att[:, h * head : (h + 1) * head] = (numer / denom).astype(jnp.bfloat16)
    share = q_ref.shape[0] // (2 * sides)
    core = core_ref[0]
    for out_ref, which in ((sent_ref, 1 - core), (kept_ref, core)):
        rows = jnp.concatenate(
            [att[pl.ds(pl.multiple_of((2 * s + which) * share, share), share), :] for s in range(sides)]
        )
        out = jnp.dot(rows, weight_ref[...], preferred_element_type=jnp.float32)
        out_ref[...] = out.astype(jnp.bfloat16)


def attend_blocks(rot_q, joined, key_heads, head):
    rows = rot_q.shape[0]
    group = rot_q.shape[1] // head // key_heads
    queries = rot_q.reshape(rows, key_heads, group, head)
    width = key_heads * head

    def fold_block(carry, block):
        highest, denom, numer = carry
        key_block = block[:, :width].reshape(-1, key_heads, head)
        value_block = block[:, width:].reshape(-1, key_heads, head)
        scores = jnp.einsum("qkgd,skd->qkgs", queries, key_block, preferred_element_type=jnp.float32)
        new_high = jnp.maximum(highest, jnp.max(scores, axis=-1))
        shrink = jnp.exp(highest - new_high)
        expo = jnp.exp(scores - new_high[..., None])
        denom = denom * shrink + jnp.sum(expo, axis=-1)
        numer = numer * shrink[..., None] + jnp.einsum(
            "qkgs,skd->qkgd",
            expo.astype(jnp.bfloat16),
            value_block,
            preferred_element_type=jnp.float32,
        )
        return ((new_high, denom, numer), None)

    shape = (rows, key_heads, group)
    carry = (
        jnp.full(shape, -1e30, jnp.float32),
        jnp.zeros(shape, jnp.float32),
        jnp.zeros(shape + (head,), jnp.float32),
    )
    length = joined.shape[0]
    size = length
    while size > 2048 and size % 2 == 0:
        size = size // 2
    blocks = joined.reshape(length // size, size, joined.shape[1])
    carry, _ = lax.scan(fold_block, carry, blocks)
    _, denom, numer = carry
    return (numer / denom[..., None]).astype(jnp.bfloat16).reshape(rows, -1)


def attention(rot_q, joined, out_weight, key_heads, head):
    near = lax.axis_size("n")
    sides = lax.axis_size("y")
    core = lax.axis_index("c").astype(jnp.int32)
    rows = rot_q.shape[0]
    width = out_weight.shape[1]
    far = swap(joined, "f")
    if near <= DIRECT_MAX:
        pair = jnp.concatenate([joined, far], axis=0)
        kvs = [pair]
        for k in [1 << b for b in reversed(range(near.bit_length() - 1))]:
            held = kvs[0] if len(kvs) == 1 else jnp.concatenate(kvs, axis=0)
            kvs = [held, swap(held, "n", k)]
        body = functools.partial(attend_body, head=head, key_heads=key_heads, sides=sides)
        half = ((rows // 2, width), jnp.bfloat16)
        return call(
            body,
            [half, half],
            [SMEM, WHOLE] + [VMEM] * len(kvs) + [WHOLE],
            (core.reshape(1), rot_q, *kvs, out_weight),
            [pltpu.VMEM(rot_q.shape, jnp.bfloat16)],
            micros=5.0,
            mib=24,
        )
    pair = jnp.concatenate([joined, far], axis=0)
    joined = lax.all_gather(pair, "n", axis=0, tiled=True)
    attended = attend_blocks(rot_q, joined, key_heads, head)
    blocks = attended.reshape(sides, 2, -1, attended.shape[1])

    def project(which):
        part = lax.dynamic_index_in_dim(blocks, which, 1, False).reshape(rows // 2, -1)
        out = jnp.dot(part, out_weight, preferred_element_type=jnp.float32)
        return out.astype(jnp.bfloat16)

    return project(1 - core), project(core)


def finish_mixer(sent, kept):
    sides = lax.axis_size("y")
    pair = kept.astype(jnp.float32) + swap(sent, "c").astype(jnp.float32)
    pair = pair.reshape(sides, -1, kept.shape[1])
    if sides == 1:
        return pair[0].astype(jnp.bfloat16)
    if sides == 2:
        side = lax.axis_index("y")
        sent = lax.dynamic_index_in_dim(pair, 1 - side, 0, False).astype(jnp.bfloat16)
        kept = lax.dynamic_index_in_dim(pair, side, 0, False)
        return (kept + swap(sent, "y").astype(jnp.float32)).astype(jnp.bfloat16)
    moved = lax.all_to_all(pair.astype(jnp.bfloat16), "y", 0, 0, tiled=True)
    return jnp.sum(moved.astype(jnp.float32), axis=0).astype(jnp.bfloat16)


def local(
    queries,
    keys,
    values,
    q_gain,
    k_gain,
    out_weight,
    tokens,
    ffn_gain,
    route,
    route_weight,
    gate_weight,
    up_weight,
    down_weight,
):
    bf16 = jnp.bfloat16
    near = lax.axis_size("n")
    sides = lax.axis_size("y")
    half = lax.axis_index("f").astype(jnp.int32)
    here = half * near + lax.axis_index("n").astype(jnp.int32)
    base = (half * near).reshape(1)

    own_rows, width = tokens.shape
    top = route.shape[1]
    capacity = own_rows * top // near
    sizes = (near, sides, capacity, top)
    slots = near * sides * capacity
    send = functools.partial(send_body, sizes=sizes)
    outgoing, near_rows = call(
        send, [((own_rows, width + LANES), bf16), ((slots, width), bf16)], [SMEM] + [WHOLE] * 4,
        (base, tokens, ffn_gain.reshape(1, -1), route.T, route_weight.T), micros=1.5)
    far = swap(outgoing, "f")
    near_in = exchange(near_rows, capacity)
    relay = functools.partial(relay_body, sizes=sizes)
    (far_rows,) = call(relay, [((slots, width), bf16)], [SMEM, VMEM], (base, far))
    far_in = exchange(far_rows, capacity)

    local_rows = queries.shape[0]
    head = q_gain.shape[0]
    row_table, col_table = turn_tables(local_rows * 2 * near // GRID_W, head)
    rot_q, joined = call(
        qkv_body,
        [(queries.shape, bf16), ((local_rows, 2 * keys.shape[1]), bf16)],
        [SMEM] + [WHOLE] * 7 + [VMEM],
        (
            (here * (local_rows // GRID_W)).reshape(1),
            queries,
            keys.T,
            values.T,
            q_gain.reshape(1, -1),
            k_gain.reshape(1, -1),
            row_table,
            col_table,
            near_rows,
        ),
        micros=1.5,
    )

    weights = (gate_weight, up_weight, down_weight)

    def work(rows):
        mine, other = run_expert(rows, swap(rows, "c"), *weights)
        args = (mine, swap(other, "c"))
        return call(add_body, [(rows.shape, bf16)], [VMEM] * 2, args)[0]

    near_out = work(near_in)
    far_out = work(far_in)
    far_back = exchange(far_out, capacity)
    near_back = exchange(near_out, capacity)

    sent, kept = attention(rot_q, joined, out_weight, keys.shape[1] // head, head)
    mixer_out = finish_mixer(sent, kept)

    collect = functools.partial(collect_body, sizes=sizes)

    def gather_back(meta, back, dtype):
        return call(
            collect, [((own_rows, width), dtype)], [SMEM, VMEM, VMEM], (base, meta, back)
        )[0]

    far_sum = swap(gather_back(far, far_back, bf16), "f")
    near_sum = gather_back(outgoing, near_back, jnp.float32)
    mixed = (near_sum + far_sum.astype(jnp.float32)).astype(bf16)
    return (mixer_out, mixed)


def solution(mesh):
    devices = mesh.devices
    groups, parts = devices.shape
    split = Mesh(devices.reshape(2, groups // 2, parts // 2, 2), ("f", "n", "y", "c"))
    ep = ("f", "n")
    tp = ("y", "c")
    placed = (
        P(ep, tp),
        P(ep, tp),
        P(ep, tp),
        P(),
        P(),
        P(tp, None),
        P(ep + tp, None),
        P(),
        P(ep + tp, None),
        P(ep + tp, None),
        P(ep, None, tp),
        P(ep, None, tp),
        P(ep, tp, None),
    )
    return jax.shard_map(
        local,
        mesh=split,
        in_specs=placed,
        out_specs=(P(ep + tp, None), P(ep + tp, None)),
        check_vma=False,
    )
```
